128 devices in a mesh: fs: 16 (over z, y), tp: 8 (over x, core).
Axes of the slice: x: 4, y: 4, z: 4, core: 2. Of those that a mesh axis runs over, the one named last changes fastest.
Arguments:
- inputs: bfloat16 [8192, 3072], P('fs', 'tp'), may hold values from -6 to 6
- cotangent: bfloat16 [8192, 3072], P('fs', 'tp'), may hold values from -6 to 6
- pre_norm: bfloat16 [8192, 3072], P('fs', 'tp'), may hold values from -28 to 28, as said below
- gate_pre: bfloat16 [8192, 5632], P('fs', 'tp'), may hold values from -8 to 8
- value_pre: bfloat16 [8192, 5632], P('fs', 'tp'), may hold values from -6 to 6
- gate_weight: bfloat16 [3072, 5632], P('fs', 'tp'), may hold values from -0.109375 to 0.109375
- value_weight: bfloat16 [3072, 5632], P('fs', 'tp'), may hold values from -0.109375 to 0.109375
- down_weight: bfloat16 [5632, 3072], P('tp', 'fs'), may hold values from -0.078125 to 0.078125
- conv_taps: float32 [3, 5632], P(None, 'tp'), may hold values from -3.5 to 3.5
- norm_gain: float32 [3072], P('tp'), may hold values from 0.1 to 1.9
Outputs:
- grad_input: bfloat16 [8192, 3072], P('fs', 'tp')
- grad_gate: float32 [3072, 5632], P('fs', 'tp')
- grad_value: float32 [3072, 5632], P('fs', 'tp')
- grad_down: float32 [5632, 3072], P('tp', 'fs')
- grad_taps: float32 [3, 5632], P(None, 'tp')
- grad_gain: float32 [3072], P('tp')
The draws below stay inside these ranges and needn't reach their ends.
Inputs may be any that keep to these rules, and one draw needn't show every extreme that they name: `pre_norm`: every entry has magnitude 0.075 or more.
All inputs are finite; a program needn't handle non-finite values.
Results may differ from the reference program's by a relative error of at most 0.014.
Values may be sent and summed in bfloat16 or wider, within the bound.
No kernel may reach another device: no remote copies, remote signals or barrier semaphores. Data moves between devices by JAX's collectives and lax.ppermute only.
A program may use at most 128 MiB of HBM per device.

```python
import jax
import jax.numpy as jnp
from jax import lax

D = 3072
FF = 5632
SEQ = 128
TOKENS = 8192
N_TP = 8


def draw_pre_norm(key, part):
    base = jax.random.fold_in(key, 11)
    first, second, third, fourth = jax.random.split(base, 4)
    blocks = jnp.exp(jax.random.uniform(first, (8,), jnp.float32, jnp.log(0.3), jnp.log(3.0)))
    column_scale = jnp.repeat(blocks, D // 8)
    magnitude = 0.5 + jnp.minimum(jnp.abs(jax.random.normal(second, (TOKENS, D), jnp.float32)), 4.0)
    signs = jnp.where(jax.random.bernoulli(third, 0.5, (TOKENS, D)), 1.0, -1.0)
    row_scale = jnp.exp(jax.random.uniform(fourth, (TOKENS, 1), jnp.float32, -0.7, 0.7))
    return (signs * magnitude * column_scale[None, :] * row_scale).astype(jnp.bfloat16)


def strengthened(entries, own_key, source, target, parts, factor):
    owner, partner = [(jnp.arange(entries.shape[axis_at]) // (entries.shape[axis_at] // parts)).reshape([-1 if axis == axis_at else 1 for axis in range(entries.ndim)]) for axis_at in (source, target)]
    chosen = jax.random.permutation(own_key, parts)[partner]
    strong = (owner == chosen) | (owner == (partner + parts // 2) % parts)
    return jnp.where(strong, factor * entries, entries)


def block_scale(key, dims, cuts, low, top_value):
    level, own = 1.0, jax.random.fold_in(key, 6)
    for position, parts in cuts:
        draws = jnp.exp(jax.random.uniform(jax.random.fold_in(own, position), (parts,), jnp.float32, low / len(cuts), top_value / len(cuts)))
        level = level * jnp.repeat(draws, dims[position] // parts).reshape([-1 if axis == position else 1 for axis in range(len(dims))])
    return level


def scatter_about(rng, shape, deviation, bound, cuts=(), kind=jnp.bfloat16):
    level = block_scale(rng, shape, cuts, -0.22, 0.18) if cuts else 1.0
    drawn = jax.random.normal(rng, shape, jnp.float32) * deviation * level
    return jnp.minimum(jnp.maximum(drawn, -bound), bound).astype(kind)


def bell_draw_with(key, shape, width, most, cuts, heavy, kind=jnp.bfloat16):
    result = width * jax.random.normal(key, shape, jnp.float32)
    if cuts:
        result = result * block_scale(key, shape, cuts, -0.22, 0.18)
    return jnp.clip(strengthened(result, jax.random.fold_in(key, 3), *heavy), -most, most).astype(kind)


def setup_inputs(seed: int = 0) -> dict:
    key_of = jax.random.split(jax.random.key(seed), 11)
    inputs = scatter_about(key_of[0], (TOKENS, D), 1.0, 6.0, ((0, 16), (1, 8)))
    cotangent = bell_draw_with(key_of[1], (TOKENS, D), 1.0, 6.0, ((0, 16), (1, 8)), (0, 1, 16, 2.0))
    pre_norm = draw_pre_norm(jax.random.fold_in(key_of[10], 71), 0)
    gate_pre = scatter_about(key_of[3], (TOKENS, FF), 1.5, 8.0, ((0, 16), (1, 8)))
    value_pre = scatter_about(key_of[4], (TOKENS, FF), 1.0, 6.0, ((0, 16), (1, 8)))
    gate_weight = scatter_about(key_of[5], (D, FF), D ** -0.5, 0.109375, ((0, 16), (1, 8)))
    value_weight = scatter_about(key_of[6], (D, FF), D ** -0.5, 0.109375, ((0, 16), (1, 8)))
    down_weight = scatter_about(key_of[7], (FF, D), FF ** -0.5, 0.078125, ((0, 8), (1, 16)))
    conv_taps = scatter_about(key_of[8], (3, FF), 3 ** -0.5, 3.5, ((1, 8),), jnp.float32)
    norm_gain = jnp.clip(1.0 + 0.18 * jax.random.normal(key_of[9], (D,), jnp.float32), 0.1, 1.9)
    return {"inputs": inputs, "cotangent": cotangent, "pre_norm": pre_norm, "gate_pre": gate_pre, "value_pre": value_pre, "gate_weight": gate_weight, "value_weight": value_weight, "down_weight": down_weight, "conv_taps": conv_taps, "norm_gain": norm_gain}


EPSILON = 1e-06

def shifted(values, forward):
    positions = jnp.arange(values.shape[0]) % SEQ
    zeros_row = jnp.zeros((1, values.shape[1]), values.dtype)
    if forward:
        moved = jnp.concatenate([zeros_row, values[:-1]], axis=0)
        keep = positions != 0
    else:
        moved = jnp.concatenate([values[1:], zeros_row], axis=0)
        keep = positions != SEQ - 1
    return jnp.where(keep[:, None], moved, jnp.zeros_like(moved))

def contract_rows(left, right):
    return lax.dot_general(left, right, (((0,), (0,)), ((), ())), preferred_element_type=jnp.float32)

def reference(inputs, cotangent, pre_norm, gate_pre, value_pre, gate_weight, value_weight, down_weight, conv_taps, norm_gain):
    normed = pre_norm.astype(jnp.float32)
    cot_float = cotangent.astype(jnp.float32)
    scaled = norm_gain[None, :] * cot_float
    inverse = lax.rsqrt(lax.optimization_barrier(jnp.sum(normed * normed, axis=1)) / D + EPSILON)
    cross = lax.optimization_barrier(jnp.sum(normed * scaled, axis=1)) / D
    grad_pre = (inverse[:, None] * (scaled - normed * (inverse * inverse * cross)[:, None])).astype(jnp.bfloat16)
    grad_gain = lax.optimization_barrier(jnp.sum(cot_float * normed * inverse[:, None], axis=0))
    gate_float = gate_pre.astype(jnp.float32)
    before = shifted(gate_float, True)
    after = shifted(gate_float, False)
    mixed = conv_taps[0][None] * before + conv_taps[1][None] * gate_float + conv_taps[2][None] * after
    sig = jax.nn.sigmoid(mixed)
    active = mixed * sig
    value_float = value_pre.astype(jnp.float32)
    hidden = (active * value_float).astype(jnp.bfloat16)
    grad_act = lax.dot_general(grad_pre, down_weight, (((1,), (1,)), ((), ())), preferred_element_type=jnp.float32)
    grad_val = (grad_act * active).astype(jnp.bfloat16)
    grad_mixed = grad_act * value_float * sig * (1.0 + mixed * (1.0 - sig))
    grad_taps = jnp.stack([lax.optimization_barrier(jnp.sum(grad_mixed * before, axis=0)), lax.optimization_barrier(jnp.sum(grad_mixed * gate_float, axis=0)), lax.optimization_barrier(jnp.sum(grad_mixed * after, axis=0))], axis=0)
    grad_gpre = (conv_taps[1][None] * grad_mixed + conv_taps[0][None] * shifted(grad_mixed, False) + conv_taps[2][None] * shifted(grad_mixed, True)).astype(jnp.bfloat16)
    block_size = FF // N_TP
    accum = jnp.zeros((inputs.shape[0], D), jnp.float32)
    for block in range(N_TP):
        lower = block * block_size
        upper = lower + block_size
        partial_sum = lax.dot_general(grad_gpre[:, lower:upper], gate_weight[:, lower:upper], (((1,), (1,)), ((), ())), preferred_element_type=jnp.float32)
        partial_sum = partial_sum + lax.dot_general(grad_val[:, lower:upper], value_weight[:, lower:upper], (((1,), (1,)), ((), ())), preferred_element_type=jnp.float32)
        rounded = lax.optimization_barrier(partial_sum.astype(jnp.bfloat16))
        accum = accum + rounded.astype(jnp.float32)
    grad_input = accum.astype(jnp.bfloat16)
    grad_gate = contract_rows(inputs, grad_gpre)
    grad_value = contract_rows(inputs, grad_val)
    grad_down = contract_rows(hidden, grad_pre)
    return (grad_input, grad_gate, grad_value, grad_down, grad_taps, grad_gain)
```

```python
import functools

import jax
import jax.numpy as jnp
from jax import lax
from jax.experimental import pallas as pl
from jax.experimental.pallas import tpu as pltpu
from jax.sharding import Mesh
from jax.sharding import PartitionSpec as P

D = 3072
SEQ = 128
EPSILON = 1e-06
F32 = jnp.float32
BF16 = jnp.bfloat16
FS = ("z", "y")
TP = ("x", "c")
ROWS = 192
HALF = ROWS // 2
UNITS = 704
WIDE = 768
TOKS = 512
COLS = 384


VMEM = pl.BlockSpec(memory_space=pltpu.VMEM)
SMEM = pl.BlockSpec(memory_space=pltpu.SMEM)


def moved(value, axis, by):
    return lax.ppermute(value, axis, [(i, (i + by) % 4) for i in range(4)])


def swapped(value):
    return lax.ppermute(value, "c", [(0, 1), (1, 0)])


def gathered(own, axis, name):
    half = own.shape[0] // 2
    with jax.named_scope(name + "_near"):
        left, right = moved(own, axis, 1), moved(own, axis, -1)
    with jax.named_scope(name + "_far"):
        far_low, far_high = moved(left[:half], axis, 1), moved(right[half:], axis, -1)
    return [own, right, far_low, far_high, left]


def plus(a, b):
    return (a.astype(F32) + b.astype(F32)).astype(BF16)


def reduced(own, after, far_low, far_high, before, axis, out=BF16):
    half = far_low.shape[0]
    from_left, from_right = moved(far_low, axis, 1), moved(far_high, axis, -1)
    to_right = jnp.concatenate([plus(after[:half], from_left), after[half:]], axis=0)
    to_left = jnp.concatenate([before[:half], plus(before[half:], from_right)], axis=0)
    got_left = moved(to_right, axis, 1)
    got_right = moved(to_left, axis, -1)
    return (own.astype(F32) + got_left.astype(F32) + got_right.astype(F32)).astype(out)


def in_five(value):
    n = value.shape[0] // 8
    return (value[: 2 * n], value[2 * n : 4 * n], value[4 * n : 5 * n], value[5 * n : 6 * n], value[6 * n :])


def device_at(where, dz, dy):
    return (where[0] + dz) % 4, (where[1] + dy) % 4


def mix(gate, taps):
    lane = lax.broadcasted_iota(jnp.int32, gate.shape, 1)
    before = jnp.where(lane == 0, 0.0, pltpu.roll(gate, 1, 1))
    after = jnp.where(lane == SEQ - 1, 0.0, pltpu.roll(gate, SEQ - 1, 1))
    mixed = taps[:, 0:1] * before + taps[:, 1:2] * gate + taps[:, 2:3] * after
    return before, after, mixed, jax.nn.sigmoid(mixed)


STEP = 88


def hidden_body(gate_ref, value_ref, taps_ref, hidden_ref):
    for u in range(0, UNITS, STEP):
        rows = slice(u, u + STEP)
        taps = taps_ref[rows, :]
        for t in range(0, TOKS, SEQ):
            cols = slice(t, t + SEQ)
            _, _, mixed, sig = mix(gate_ref[rows, cols].astype(F32), taps)
            hidden_ref[rows, cols] = (mixed * sig * value_ref[rows, cols].astype(F32)).astype(BF16)


def arrange_body(where_ref, mine_ref, other_ref, out_ref):
    for c_off, ref in enumerate((mine_ref, other_ref)):
        for x_off in range(4):
            block = (where_ref[2] + x_off) % 4 * 2 + (where_ref[3] + c_off) % 2
            to = pl.multiple_of(block * COLS, COLS)
            out_ref[pl.ds(to, COLS), :] = ref[x_off * COLS : (x_off + 1) * COLS, :]


def back_body(where_ref, grad_ref, gate_ref, value_ref, taps_ref, *rest):
    refs, (out_ref, sums_ref, act_ref) = rest[:5], rest[5:]
    where = [where_ref[k] for k in range(4)]
    for dz in range(4):
        for dy in range(4):
            ref = refs[(0, 1, 2 + dy // 2, 4)[dz]]
            at = (dy % 2 if dz == 2 else dy) * ROWS
            zt, yt = device_at(where, dz, dy)
            part = lax.dot_general(
                ref[at : at + ROWS, :UNITS],
                grad_ref[pl.ds(pl.multiple_of((zt * 4 + yt) * ROWS, ROWS), ROWS), :],
                (((0,), (0,)), ((), ())),
                preferred_element_type=F32,
            )
            act_ref[...] = part if dz + dy == 0 else act_ref[...] + part
    for u in range(0, UNITS, STEP):
        rows = slice(u, u + STEP)
        taps = taps_ref[rows, :]
        sums = [jnp.zeros((STEP, SEQ), F32)] * 3
        for t in range(0, TOKS, SEQ):
            cols = slice(t, t + SEQ)
            gate = gate_ref[rows, cols].astype(F32)
            before, after, mixed, sig = mix(gate, taps)
            grad_act = act_ref[rows, cols]
            out_ref[UNITS + u : UNITS + u + STEP, cols] = (grad_act * (mixed * sig)).astype(BF16)
            inner = (
                grad_act * value_ref[rows, cols].astype(F32) * sig * (1.0 + mixed * (1.0 - sig))
            )
            sums = [s + inner * g for s, g in zip(sums, (before, gate, after))]
            lane = lax.broadcasted_iota(jnp.int32, inner.shape, 1)
            following = jnp.where(lane == SEQ - 1, 0.0, pltpu.roll(inner, SEQ - 1, 1))
            previous = jnp.where(lane == 0, 0.0, pltpu.roll(inner, 1, 1))
            out_ref[rows, cols] = (
                taps[:, 1:2] * inner + taps[:, 0:1] * following + taps[:, 2:3] * previous
            ).astype(BF16)
        for k in range(3):
            sums_ref[rows, k : k + 1] = jnp.sum(sums[k], axis=1, keepdims=True)


def product(left, right):
    return lax.dot_general(
        left, right, (((1,), (1,)), ((), ())), preferred_element_type=F32
    ).astype(BF16)


def outer_body(inputs_ref, grad_ref, both_ref, hidden_ref, out_ref):
    out_ref[:, : 2 * UNITS] = product(inputs_ref[...], both_ref[...])
    out_ref[:, 2 * UNITS :] = product(grad_ref[...], hidden_ref[...])


def input_body(where_ref, weight_ref, right_ref, kept_ref, sent_ref):
    step = pl.program_id(0)
    whole = jnp.dot(weight_ref[...], right_ref[...], preferred_element_type=F32).astype(BF16)

    @pl.when(step < 4)
    def _():
        sent_ref[...] = whole

    @pl.when(step >= 4)
    def _():
        kept_ref[...] = whole


PARAMS = pltpu.CompilerParams(vmem_limit_bytes=50 * 1024 * 1024)


def hidden_of(gate, value, taps):
    return pl.pallas_call(
        hidden_body,
        out_shape=jax.ShapeDtypeStruct((UNITS, TOKS), BF16),
        in_specs=[VMEM] * 3,
        out_specs=VMEM,
        compiler_params=PARAMS,
        name="hidden",
    )(gate, value, taps)


def arranged(where, mine, other):
    return pl.pallas_call(
        arrange_body,
        out_shape=jax.ShapeDtypeStruct((D, TOKS), BF16),
        in_specs=[SMEM, VMEM, VMEM],
        out_specs=VMEM,
        compiler_params=PARAMS,
        name="arrange",
    )(where, mine, other)


def back_of(where, grad, gate, value, taps, pieces):
    return pl.pallas_call(
        back_body,
        out_shape=(
            jax.ShapeDtypeStruct((2 * UNITS, TOKS), BF16),
            jax.ShapeDtypeStruct((UNITS, 3), F32),
        ),
        in_specs=[SMEM] + [VMEM] * 9,
        out_specs=(VMEM, VMEM),
        scratch_shapes=[pltpu.VMEM((UNITS, TOKS), F32)],
        compiler_params=PARAMS,
        cost_estimate=pl.CostEstimate(
            flops=2 * D * UNITS * TOKS, bytes_accessed=12_000_000, transcendentals=UNITS * TOKS
        ),
        name="back",
    )(where, grad, gate, value, taps, *pieces)


def outer_of(inputs, grad, both, hidden):
    return pl.pallas_call(
        outer_body,
        out_shape=jax.ShapeDtypeStruct((D, 3 * UNITS), BF16),
        grid=(8,),
        in_specs=[
            pl.BlockSpec((COLS, TOKS), lambda i: (i, 0)),
            pl.BlockSpec((COLS, TOKS), lambda i: (i, 0)),
            VMEM,
            VMEM,
        ],
        out_specs=pl.BlockSpec((COLS, 3 * UNITS), lambda i: (i, 0)),
        compiler_params=PARAMS,
        cost_estimate=pl.CostEstimate(
            flops=6 * D * UNITS * TOKS, bytes_accessed=20_000_000, transcendentals=0
        ),
        name="outer",
    )(inputs, grad, both, hidden)


def input_of(where, weight, right):
    def weight_at(i, where):
        x, c = (where[2] + i % 4) % 4, (where[3] + 1 - i // 4) % 2
        return (x * 2 + c, 0)

    shape = jax.ShapeDtypeStruct((4 * COLS, TOKS), BF16)
    return pl.pallas_call(
        input_body,
        out_shape=(shape, shape),
        grid_spec=pltpu.PrefetchScalarGridSpec(
            num_scalar_prefetch=1,
            grid=(8,),
            in_specs=[pl.BlockSpec((COLS, 2 * UNITS), weight_at), VMEM],
            out_specs=(
                pl.BlockSpec((COLS, TOKS), lambda i, w: (jnp.clip(i - 4, 0, 3), 0)),
                pl.BlockSpec((COLS, TOKS), lambda i, w: (jnp.clip(i, 0, 3), 0)),
            ),
        ),
        compiler_params=PARAMS,
        cost_estimate=pl.CostEstimate(
            flops=4 * D * UNITS * TOKS, bytes_accessed=15_000_000, transcendentals=0
        ),
        name="grad_input",
    )(where, weight, right)


def copy_for_each(value, axis):
    copies = jnp.broadcast_to(value, (lax.axis_size(axis), *value.shape))
    return lax.all_to_all(copies, axis, split_axis=0, concat_axis=0, tiled=True)


def over_features(where, own, name):
    mine = jnp.concatenate(gathered(own, "x", name), axis=0)
    with jax.named_scope(name + "_swap"):
        other = swapped(mine)
    return arranged(where, mine, other)


def on_device(
    inputs,
    cotangent,
    pre_norm,
    gate_pre,
    value_pre,
    gate_weight,
    value_weight,
    down_weight,
    conv_taps,
    norm_gain,
):
    where = jnp.stack([lax.axis_index(a) for a in ("z", "y", "x", "c")]).astype(jnp.int32)
    line = jnp.concatenate(gathered(jnp.pad(down_weight.T, ((0, 0), (0, WIDE - UNITS))), "y", "down_y"), axis=0)
    down_pieces = gathered(line, "z", "down_z")
    inputs_full = over_features(where, inputs.T, "inputs")
    weights = jnp.concatenate([gate_weight, value_weight], axis=1)
    weights_full = lax.all_gather(weights, FS, axis=0, tiled=True)

    normed = pre_norm.astype(F32)
    cot_float = cotangent.astype(F32)
    scaled = norm_gain[None, :] * cot_float
    sums = jnp.concatenate([jnp.sum(normed * normed, axis=1), jnp.sum(normed * scaled, axis=1)])
    sums = jnp.sum(copy_for_each(sums, TP), axis=0)
    inverse = lax.rsqrt(sums[:TOKS] / D + EPSILON)
    cross = sums[TOKS:] / D
    grad_pre = (inverse[:, None] * (scaled - normed * (inverse * inverse * cross)[:, None])).astype(
        BF16
    )
    gain_local = jnp.sum(cot_float * normed * inverse[:, None], axis=0)

    grad_full = over_features(where, grad_pre.T, "grad")

    gate, value, taps = gate_pre.T, value_pre.T, conv_taps.T
    hidden = hidden_of(gate, value, taps)
    grads, taps_local = back_of(where, grad_full, gate, value, taps, down_pieces)
    terms = outer_of(inputs_full, grad_full, grads, hidden)
    summed = lax.psum_scatter(terms, FS, scatter_dimension=0, tiled=True).astype(F32)

    kept, sent = input_of(where, weights_full, grads)
    paired = plus(kept, swapped(sent))
    grad_input = reduced(*in_five(paired), "x", F32).T.astype(BF16)

    small = jnp.concatenate([taps_local.T.ravel(), gain_local])
    small = jnp.sum(copy_for_each(small, FS), axis=0)
    grad_taps = small[: 3 * UNITS].reshape(3, UNITS)
    grad_gain = small[3 * UNITS :]
    return (
        grad_input,
        summed[:, :UNITS],
        summed[:, UNITS : 2 * UNITS],
        summed[:, 2 * UNITS :].T,
        grad_taps,
        grad_gain,
    )


def solution(mesh):
    split = Mesh(mesh.devices.reshape(4, 4, 4, 2), ("z", "y", "x", "c"))
    in_specs = (
        P(FS, TP),
        P(FS, TP),
        P(FS, TP),
        P(FS, TP),
        P(FS, TP),
        P(FS, TP),
        P(FS, TP),
        P(TP, FS),
        P(None, TP),
        P(TP),
    )
    out_specs = (P(FS, TP), P(FS, TP), P(FS, TP), P(TP, FS), P(None, TP), P(TP))
    return jax.shard_map(
        on_device, mesh=split, in_specs=in_specs, out_specs=out_specs, check_vma=False
    )
```

```python
import jax
import jax.numpy as jnp
from jax import lax
from jax.experimental import pallas as pl
from jax.experimental.pallas import tpu as pltpu
from jax.sharding import Mesh
from jax.sharding import PartitionSpec as P


D = 3072
SEQ = 128
EPSILON = 1e-06
F32 = jnp.float32
BF16 = jnp.bfloat16
FS = ("z", "y")
TP = ("x", "c")
ROWS = 192
HALF = ROWS // 2
UNITS = 704
WIDE = 768
TOKS = 512
COLS = 384


VMEM = pl.BlockSpec(memory_space=pltpu.VMEM)
SMEM = pl.BlockSpec(memory_space=pltpu.SMEM)


def moved(value, axis, by):
    return lax.ppermute(value, axis, [(i, (i + by) % 4) for i in range(4)])


def swapped(value):
    return lax.ppermute(value, "c", [(0, 1), (1, 0)])


def gathered(own, axis):
    half = own.shape[0] // 2
    left, right = moved(own, axis, 1), moved(own, axis, -1)
    far_low, far_high = moved(left[:half], axis, 1), moved(right[half:], axis, -1)
    return [own, right, far_low, far_high, left]


def plus(a, b):
    return (a.astype(F32) + b.astype(F32)).astype(BF16)


def reduced(own, after, far_low, far_high, before, axis, out=BF16):
    half = far_low.shape[0]
    from_left, from_right = moved(far_low, axis, 1), moved(far_high, axis, -1)
    to_right = jnp.concatenate([plus(after[:half], from_left), after[half:]], axis=0)
    to_left = jnp.concatenate([before[:half], plus(before[half:], from_right)], axis=0)
    got_left = moved(to_right, axis, 1)
    got_right = moved(to_left, axis, -1)
    return (own.astype(F32) + got_left.astype(F32) + got_right.astype(F32)).astype(out)


def in_five(value):
    n = value.shape[0] // 8
    return (value[: 2 * n], value[2 * n : 4 * n], value[4 * n : 5 * n], value[5 * n : 6 * n], value[6 * n :])


def device_at(where, dz, dy):
    return (where[0] + dz) % 4, (where[1] + dy) % 4


def mix(gate, taps):
    lane = lax.broadcasted_iota(jnp.int32, gate.shape, 1)
    before = jnp.where(lane == 0, 0.0, pltpu.roll(gate, 1, 1))
    after = jnp.where(lane == SEQ - 1, 0.0, pltpu.roll(gate, SEQ - 1, 1))
    mixed = taps[:, 0:1] * before + taps[:, 1:2] * gate + taps[:, 2:3] * after
    return before, after, mixed, jax.nn.sigmoid(mixed)


STEP = 88


def hidden_body(gate_ref, value_ref, taps_ref, hidden_ref):
    for u in range(0, UNITS, STEP):
        rows = slice(u, u + STEP)
        taps = taps_ref[rows, :]
        for t in range(0, TOKS, SEQ):
            cols = slice(t, t + SEQ)
            _, _, mixed, sig = mix(gate_ref[rows, cols].astype(F32), taps)
            hidden_ref[rows, cols] = (mixed * sig * value_ref[rows, cols].astype(F32)).astype(BF16)


def arrange_body(where_ref, mine_ref, other_ref, out_ref):
    for c_off, ref in enumerate((mine_ref, other_ref)):
        for x_off in range(4):
            block = (where_ref[2] + x_off) % 4 * 2 + (where_ref[3] + c_off) % 2
            to = pl.multiple_of(block * COLS, COLS)
            out_ref[pl.ds(to, COLS), :] = ref[x_off * COLS : (x_off + 1) * COLS, :]


def back_body(down_ref, grad_ref, gate_ref, value_ref, taps_ref, out_ref, sums_ref, act_ref):
    act_ref[...] = lax.dot_general(
        down_ref[:, :UNITS],
        grad_ref[...],
        (((0,), (0,)), ((), ())),
        preferred_element_type=F32,
    )
    for u in range(0, UNITS, STEP):
        rows = slice(u, u + STEP)
        taps = taps_ref[rows, :]
        sums = [jnp.zeros((STEP, SEQ), F32)] * 3
        for t in range(0, TOKS, SEQ):
            cols = slice(t, t + SEQ)
            gate = gate_ref[rows, cols].astype(F32)
            before, after, mixed, sig = mix(gate, taps)
            grad_act = act_ref[rows, cols]
            out_ref[UNITS + u : UNITS + u + STEP, cols] = (grad_act * (mixed * sig)).astype(BF16)
            inner = (
                grad_act * value_ref[rows, cols].astype(F32) * sig * (1.0 + mixed * (1.0 - sig))
            )
            sums = [s + inner * g for s, g in zip(sums, (before, gate, after))]
            lane = lax.broadcasted_iota(jnp.int32, inner.shape, 1)
            following = jnp.where(lane == SEQ - 1, 0.0, pltpu.roll(inner, SEQ - 1, 1))
            previous = jnp.where(lane == 0, 0.0, pltpu.roll(inner, 1, 1))
            out_ref[rows, cols] = (
                taps[:, 1:2] * inner + taps[:, 0:1] * following + taps[:, 2:3] * previous
            ).astype(BF16)
        for k in range(3):
            sums_ref[rows, k : k + 1] = jnp.sum(sums[k], axis=1, keepdims=True)


def product(left, right):
    return lax.dot_general(
        left, right, (((1,), (1,)), ((), ())), preferred_element_type=F32
    ).astype(BF16)


def outer_body(inputs_ref, grad_ref, both_ref, hidden_ref, out_ref):
    out_ref[:, : 2 * UNITS] = product(inputs_ref[...], both_ref[...])
    out_ref[:, 2 * UNITS :] = product(grad_ref[...], hidden_ref[...])


def block_of(refs, dz, dy):
    def part(five, major, minor):
        ref = five[(0, 1, 2 + minor // 2, 4)[major]]
        at = (minor % 2 if major == 2 else minor) * HALF
        return ref[at : at + HALF, :]

    return jnp.concatenate([part(refs[:5], dz, dy), part(refs[5:], dy, dz)], axis=0)


def input_body(where_ref, right_ref, *rest):
    refs, (kept_ref, sent_ref) = rest[:10], rest[10:]
    where = [where_ref[k] for k in range(4)]
    for dz in range(4):
        for dy in range(4):
            zt, yt = device_at(where, dz, dy)
            at = pl.multiple_of((((zt - where[2] + 4) % 4) * 2 + yt % 2) * ROWS, ROWS)
            near = yt // 2 == where[3]
            block = jnp.dot(
                block_of(refs, dz, dy), right_ref[...], preferred_element_type=F32
            ).astype(BF16)

            @pl.when(near)
            def _():
                kept_ref[pl.ds(at, ROWS), :] = block

            @pl.when(jnp.logical_not(near))
            def _():
                sent_ref[pl.ds(at, ROWS), :] = block


PARAMS = pltpu.CompilerParams(vmem_limit_bytes=50 * 1024 * 1024)


def hidden_of(gate, value, taps):
    return pl.pallas_call(
        hidden_body,
        out_shape=jax.ShapeDtypeStruct((UNITS, TOKS), BF16),
        in_specs=[VMEM] * 3,
        out_specs=VMEM,
        compiler_params=PARAMS,
        name="hidden",
    )(gate, value, taps)


def arranged(where, mine, other):
    return pl.pallas_call(
        arrange_body,
        out_shape=jax.ShapeDtypeStruct((D, TOKS), BF16),
        in_specs=[SMEM, VMEM, VMEM],
        out_specs=VMEM,
        compiler_params=PARAMS,
        name="arrange",
    )(where, mine, other)


def back_of(down, grad, gate, value, taps):
    return pl.pallas_call(
        back_body,
        out_shape=(
            jax.ShapeDtypeStruct((2 * UNITS, TOKS), BF16),
            jax.ShapeDtypeStruct((UNITS, 3), F32),
        ),
        in_specs=[VMEM] * 5,
        out_specs=(VMEM, VMEM),
        scratch_shapes=[pltpu.VMEM((UNITS, TOKS), F32)],
        compiler_params=PARAMS,
        cost_estimate=pl.CostEstimate(
            flops=2 * D * UNITS * TOKS, bytes_accessed=12_000_000, transcendentals=UNITS * TOKS
        ),
        name="back",
    )(down, grad, gate, value, taps)


def outer_of(inputs, grad, both, hidden):
    return pl.pallas_call(
        outer_body,
        out_shape=jax.ShapeDtypeStruct((D, 3 * UNITS), BF16),
        grid=(8,),
        in_specs=[
            pl.BlockSpec((COLS, TOKS), lambda i: (i, 0)),
            pl.BlockSpec((COLS, TOKS), lambda i: (i, 0)),
            VMEM,
            VMEM,
        ],
        out_specs=pl.BlockSpec((COLS, 3 * UNITS), lambda i: (i, 0)),
        compiler_params=PARAMS,
        cost_estimate=pl.CostEstimate(
            flops=6 * D * UNITS * TOKS, bytes_accessed=20_000_000, transcendentals=0
        ),
        name="outer",
    )(inputs, grad, both, hidden)


def input_of(where, right, pieces):
    shape = jax.ShapeDtypeStruct((4 * COLS, TOKS), BF16)
    return pl.pallas_call(
        input_body,
        out_shape=(shape, shape),
        in_specs=[SMEM] + [VMEM] * 11,
        out_specs=(VMEM, VMEM),
        compiler_params=PARAMS,
        cost_estimate=pl.CostEstimate(
            flops=4 * D * UNITS * TOKS, bytes_accessed=15_000_000, transcendentals=0
        ),
        name="grad_input",
    )(where, right, *pieces)


def copy_for_each(value, axis):
    copies = jnp.broadcast_to(value, (lax.axis_size(axis), *value.shape))
    return lax.all_to_all(copies, axis, split_axis=0, concat_axis=0, tiled=True)


def over_features(where, own):
    mine = jnp.concatenate(gathered(own, "x"), axis=0)
    other = swapped(mine)
    return arranged(where, mine, other)


def layer(
    inputs,
    cotangent,
    pre_norm,
    gate_pre,
    value_pre,
    gate_weight,
    value_weight,
    down_weight,
    conv_taps,
    norm_gain,
):
    where = jnp.stack([lax.axis_index(a) for a in ("z", "y", "x", "c")]).astype(jnp.int32)
    down = jnp.pad(down_weight.T, ((0, 0), (0, WIDE - UNITS)))
    down_full = lax.all_gather(down, FS, axis=0, tiled=True)
    inputs_full = over_features(where, inputs.T)
    weights = jnp.concatenate([gate_weight, value_weight], axis=1)
    top = jnp.concatenate(gathered(weights[:HALF], "y"), axis=0)
    low = jnp.concatenate(gathered(weights[HALF:], "z"), axis=0)

    normed = pre_norm.astype(F32)
    cot_float = cotangent.astype(F32)
    scaled = norm_gain[None, :] * cot_float
    sums = jnp.concatenate([jnp.sum(normed * normed, axis=1), jnp.sum(normed * scaled, axis=1)])
    sums = jnp.sum(copy_for_each(sums, TP), axis=0)
    inverse = lax.rsqrt(sums[:TOKS] / D + EPSILON)
    cross = sums[TOKS:] / D
    grad_pre = (inverse[:, None] * (scaled - normed * (inverse * inverse * cross)[:, None])).astype(
        BF16
    )
    gain_local = jnp.sum(cot_float * normed * inverse[:, None], axis=0)

    grad_full = over_features(where, grad_pre.T)

    gate, value, taps = gate_pre.T, value_pre.T, conv_taps.T
    gate, top, low = lax.optimization_barrier((gate, top, low))
    pieces = (*gathered(top, "z"), *gathered(low, "y"))
    hidden = hidden_of(gate, value, taps)
    grads, taps_local = back_of(down_full, grad_full, gate, value, taps)
    terms = outer_of(inputs_full, grad_full, grads, hidden)
    summed = lax.psum_scatter(terms, FS, scatter_dimension=0, tiled=True).astype(F32)

    kept, sent = input_of(where, grads, pieces)
    paired = plus(kept, swapped(sent))
    grad_input = reduced(*in_five(paired), "x", F32).T.astype(BF16)

    small = jnp.concatenate([taps_local.T.ravel(), gain_local])
    small = jnp.sum(copy_for_each(small, FS), axis=0)
    grad_taps = small[: 3 * UNITS].reshape(3, UNITS)
    grad_gain = small[3 * UNITS :]
    return (
        grad_input,
        summed[:, :UNITS],
        summed[:, UNITS : 2 * UNITS],
        summed[:, 2 * UNITS :].T,
        grad_taps,
        grad_gain,
    )


def solution(mesh):
    split = Mesh(mesh.devices.reshape(4, 4, 4, 2), ("z", "y", "x", "c"))
    in_specs = (
        P(FS, TP),
        P(FS, TP),
        P(FS, TP),
        P(FS, TP),
        P(FS, TP),
        P(FS, TP),
        P(FS, TP),
        P(TP, FS),
        P(None, TP),
        P(TP),
    )
    out_specs = (P(FS, TP), P(FS, TP), P(FS, TP), P(TP, FS), P(None, TP), P(TP))
    return jax.shard_map(layer, mesh=split, in_specs=in_specs, out_specs=out_specs, check_vma=False)
```

```python
import jax
import jax.numpy as jnp
from jax import lax
from jax.experimental import pallas as pl
from jax.experimental.pallas import tpu as pltpu
from jax.sharding import Mesh
from jax.sharding import PartitionSpec as P


D = 3072
SEQ = 128
EPSILON = 1e-06
F32 = jnp.float32
BF16 = jnp.bfloat16
FS = ("z", "y")
TP = ("x", "c")
ROWS = 192
HALF = ROWS // 2
UNITS = 704
WIDE = 768
TOKS = 512
COLS = 384


VMEM = pl.BlockSpec(memory_space=pltpu.VMEM)
SMEM = pl.BlockSpec(memory_space=pltpu.SMEM)


def moved(value, axis, by):
    return lax.ppermute(value, axis, [(i, (i + by) % 4) for i in range(4)])


def swapped(value):
    return lax.ppermute(value, "c", [(0, 1), (1, 0)])


def gathered(own, axis):
    half = own.shape[0] // 2
    left, right = moved(own, axis, 1), moved(own, axis, -1)
    far_low, far_high = moved(left[:half], axis, 1), moved(right[half:], axis, -1)
    return [own, right, far_low, far_high, left]


def plus(a, b):
    return (a.astype(F32) + b.astype(F32)).astype(BF16)


def reduced(own, after, far_low, far_high, before, axis, out=BF16):
    half = far_low.shape[0]
    from_left, from_right = moved(far_low, axis, 1), moved(far_high, axis, -1)
    to_right = jnp.concatenate([plus(after[:half], from_left), after[half:]], axis=0)
    to_left = jnp.concatenate([before[:half], plus(before[half:], from_right)], axis=0)
    got_left = moved(to_right, axis, 1)
    got_right = moved(to_left, axis, -1)
    return (own.astype(F32) + got_left.astype(F32) + got_right.astype(F32)).astype(out)


def in_five(value):
    n = value.shape[0] // 8
    return (value[: 2 * n], value[2 * n : 4 * n], value[4 * n : 5 * n], value[5 * n : 6 * n], value[6 * n :])


def device_at(where, dz, dy):
    return (where[0] + dz) % 4, (where[1] + dy) % 4


def mix(gate, taps):
    lane = lax.broadcasted_iota(jnp.int32, gate.shape, 1)
    before = jnp.where(lane == 0, 0.0, pltpu.roll(gate, 1, 1))
    after = jnp.where(lane == SEQ - 1, 0.0, pltpu.roll(gate, SEQ - 1, 1))
    mixed = taps[:, 0:1] * before + taps[:, 1:2] * gate + taps[:, 2:3] * after
    return before, after, mixed, jax.nn.sigmoid(mixed)


STEP = 88


def hidden_body(gate_ref, value_ref, taps_ref, hidden_ref):
    for u in range(0, UNITS, STEP):
        rows = slice(u, u + STEP)
        taps = taps_ref[rows, :]
        for t in range(0, TOKS, SEQ):
            cols = slice(t, t + SEQ)
            _, _, mixed, sig = mix(gate_ref[rows, cols].astype(F32), taps)
            hidden_ref[rows, cols] = (mixed * sig * value_ref[rows, cols].astype(F32)).astype(BF16)


def arrange_body(where_ref, mine_ref, other_ref, grad_ref, inputs_ref):
    for c_off, ref in enumerate((mine_ref, other_ref)):
        for x_off in range(4):
            block = (where_ref[2] + x_off) % 4 * 2 + (where_ref[3] + c_off) % 2
            to = pl.multiple_of(block * COLS, COLS)
            at = x_off * COLS
            grad_ref[pl.ds(to, COLS), :] = ref[at : at + COLS, :TOKS]
            inputs_ref[pl.ds(to, COLS), :] = ref[at : at + COLS, TOKS:]


def back_body(down_ref, grad_ref, gate_ref, value_ref, taps_ref, out_ref, sums_ref, act_ref):
    act_ref[...] = lax.dot_general(
        down_ref[:, :UNITS],
        grad_ref[...],
        (((0,), (0,)), ((), ())),
        preferred_element_type=F32,
    )
    for u in range(0, UNITS, STEP):
        rows = slice(u, u + STEP)
        taps = taps_ref[rows, :]
        sums = [jnp.zeros((STEP, SEQ), F32)] * 3
        for t in range(0, TOKS, SEQ):
            cols = slice(t, t + SEQ)
            gate = gate_ref[rows, cols].astype(F32)
            before, after, mixed, sig = mix(gate, taps)
            grad_act = act_ref[rows, cols]
            out_ref[UNITS + u : UNITS + u + STEP, cols] = (grad_act * (mixed * sig)).astype(BF16)
            inner = (
                grad_act * value_ref[rows, cols].astype(F32) * sig * (1.0 + mixed * (1.0 - sig))
            )
            sums = [s + inner * g for s, g in zip(sums, (before, gate, after))]
            lane = lax.broadcasted_iota(jnp.int32, inner.shape, 1)
            following = jnp.where(lane == SEQ - 1, 0.0, pltpu.roll(inner, SEQ - 1, 1))
            previous = jnp.where(lane == 0, 0.0, pltpu.roll(inner, 1, 1))
            out_ref[rows, cols] = (
                taps[:, 1:2] * inner + taps[:, 0:1] * following + taps[:, 2:3] * previous
            ).astype(BF16)
        for k in range(3):
            sums_ref[rows, k : k + 1] = jnp.sum(sums[k], axis=1, keepdims=True)


def product(left, right):
    return lax.dot_general(
        left, right, (((1,), (1,)), ((), ())), preferred_element_type=F32
    ).astype(BF16)


def outer_body(inputs_ref, grad_ref, both_ref, hidden_ref, out_ref):
    out_ref[:, : 2 * UNITS] = product(inputs_ref[...], both_ref[...])
    out_ref[:, 2 * UNITS :] = product(grad_ref[...], hidden_ref[...])


def block_of(refs, dz, dy):
    def part(five, major, minor):
        ref = five[(0, 1, 2 + minor // 2, 4)[major]]
        at = (minor % 2 if major == 2 else minor) * HALF
        return ref[at : at + HALF, :]

    return jnp.concatenate([part(refs[:5], dz, dy), part(refs[5:], dy, dz)], axis=0)


def input_body(where_ref, right_ref, *rest):
    refs, (kept_ref, sent_ref) = rest[:10], rest[10:]
    where = [where_ref[k] for k in range(4)]
    for dz in range(4):
        for dy in range(4):
            zt, yt = device_at(where, dz, dy)
            at = pl.multiple_of((((zt - where[2] + 4) % 4) * 2 + yt % 2) * ROWS, ROWS)
            near = yt // 2 == where[3]
            block = jnp.dot(
                block_of(refs, dz, dy), right_ref[...], preferred_element_type=F32
            ).astype(BF16)

            @pl.when(near)
            def _():
                kept_ref[pl.ds(at, ROWS), :] = block

            @pl.when(jnp.logical_not(near))
            def _():
                sent_ref[pl.ds(at, ROWS), :] = block


PARAMS = pltpu.CompilerParams(vmem_limit_bytes=50 * 1024 * 1024)


def hidden_of(gate, value, taps):
    return pl.pallas_call(
        hidden_body,
        out_shape=jax.ShapeDtypeStruct((UNITS, TOKS), BF16),
        in_specs=[VMEM] * 3,
        out_specs=VMEM,
        compiler_params=PARAMS,
        name="hidden",
    )(gate, value, taps)


def arranged(where, mine, other):
    shape = jax.ShapeDtypeStruct((D, TOKS), BF16)
    return pl.pallas_call(
        arrange_body,
        out_shape=(shape, shape),
        in_specs=[SMEM, VMEM, VMEM],
        out_specs=(VMEM, VMEM),
        compiler_params=PARAMS,
        name="arrange",
    )(where, mine, other)


def back_of(down, grad, gate, value, taps):
    return pl.pallas_call(
        back_body,
        out_shape=(
            jax.ShapeDtypeStruct((2 * UNITS, TOKS), BF16),
            jax.ShapeDtypeStruct((UNITS, 3), F32),
        ),
        in_specs=[VMEM] * 5,
        out_specs=(VMEM, VMEM),
        scratch_shapes=[pltpu.VMEM((UNITS, TOKS), F32)],
        compiler_params=PARAMS,
        cost_estimate=pl.CostEstimate(
            flops=2 * D * UNITS * TOKS, bytes_accessed=12_000_000, transcendentals=UNITS * TOKS
        ),
        name="back",
    )(down, grad, gate, value, taps)


def outer_of(inputs, grad, both, hidden):
    return pl.pallas_call(
        outer_body,
        out_shape=jax.ShapeDtypeStruct((D, 3 * UNITS), BF16),
        grid=(8,),
        in_specs=[
            pl.BlockSpec((COLS, TOKS), lambda i: (i, 0)),
            pl.BlockSpec((COLS, TOKS), lambda i: (i, 0)),
            VMEM,
            VMEM,
        ],
        out_specs=pl.BlockSpec((COLS, 3 * UNITS), lambda i: (i, 0)),
        compiler_params=PARAMS,
        cost_estimate=pl.CostEstimate(
            flops=6 * D * UNITS * TOKS, bytes_accessed=20_000_000, transcendentals=0
        ),
        name="outer",
    )(inputs, grad, both, hidden)


def input_of(where, right, pieces):
    shape = jax.ShapeDtypeStruct((4 * COLS, TOKS), BF16)
    return pl.pallas_call(
        input_body,
        out_shape=(shape, shape),
        in_specs=[SMEM] + [VMEM] * 11,
        out_specs=(VMEM, VMEM),
        compiler_params=PARAMS,
        cost_estimate=pl.CostEstimate(
            flops=4 * D * UNITS * TOKS, bytes_accessed=15_000_000, transcendentals=0
        ),
        name="grad_input",
    )(where, right, *pieces)


def copy_for_each(value, axis):
    copies = jnp.broadcast_to(value, (lax.axis_size(axis), *value.shape))
    return lax.all_to_all(copies, axis, split_axis=0, concat_axis=0, tiled=True)


def over_features(where, own):
    mine = jnp.concatenate(gathered(own, "x"), axis=0)
    other = swapped(mine)
    return arranged(where, mine, other)


def layer(
    inputs,
    cotangent,
    pre_norm,
    gate_pre,
    value_pre,
    gate_weight,
    value_weight,
    down_weight,
    conv_taps,
    norm_gain,
):
    where = jnp.stack([lax.axis_index(a) for a in ("z", "y", "x", "c")]).astype(jnp.int32)
    down = jnp.pad(down_weight.T, ((0, 0), (0, WIDE - UNITS)))
    down_full = lax.all_gather(down, FS, axis=0, tiled=True)
    weights = jnp.concatenate([gate_weight, value_weight], axis=1)
    top = jnp.concatenate(gathered(weights[:HALF], "y"), axis=0)
    low = jnp.concatenate(gathered(weights[HALF:], "z"), axis=0)

    normed = pre_norm.astype(F32)
    cot_float = cotangent.astype(F32)
    scaled = norm_gain[None, :] * cot_float
    sums = jnp.concatenate([jnp.sum(normed * normed, axis=1), jnp.sum(normed * scaled, axis=1)])
    sums = copy_for_each(sums, TP)
    sums = jnp.sum(sums, axis=0)
    inverse = lax.rsqrt(sums[:TOKS] / D + EPSILON)
    cross = sums[TOKS:] / D
    grad_pre = (inverse[:, None] * (scaled - normed * (inverse * inverse * cross)[:, None])).astype(
        BF16
    )
    gain_local = jnp.sum(cot_float * normed * inverse[:, None], axis=0)

    both = jnp.concatenate([grad_pre.T, inputs.T], axis=1)
    grad_full, inputs_full = over_features(where, both)

    gate, value, taps = gate_pre.T, value_pre.T, conv_taps.T
    pieces = (*gathered(top, "z"), *gathered(low, "y"))
    hidden = hidden_of(gate, value, taps)
    grads, taps_local = back_of(down_full, grad_full, gate, value, taps)
    terms = outer_of(inputs_full, grad_full, grads, hidden)
    summed = lax.psum_scatter(terms, FS, scatter_dimension=0, tiled=True).astype(F32)

    kept, sent = input_of(where, grads, pieces)
    paired = plus(kept, swapped(sent))
    grad_input = reduced(*in_five(paired), "x", F32).T.astype(BF16)

    small = jnp.concatenate([taps_local.T.ravel(), gain_local])
    small = jnp.sum(copy_for_each(small, FS), axis=0)
    grad_taps = small[: 3 * UNITS].reshape(3, UNITS)
    grad_gain = small[3 * UNITS :]
    return (
        grad_input,
        summed[:, :UNITS],
        summed[:, UNITS : 2 * UNITS],
        summed[:, 2 * UNITS :].T,
        grad_taps,
        grad_gain,
    )


def solution(mesh):
    split = Mesh(mesh.devices.reshape(4, 4, 4, 2), ("z", "y", "x", "c"))
    in_specs = (
        P(FS, TP),
        P(FS, TP),
        P(FS, TP),
        P(FS, TP),
        P(FS, TP),
        P(FS, TP),
        P(FS, TP),
        P(TP, FS),
        P(None, TP),
        P(TP),
    )
    out_specs = (P(FS, TP), P(FS, TP), P(FS, TP), P(TP, FS), P(None, TP), P(TP))
    return jax.shard_map(layer, mesh=split, in_specs=in_specs, out_specs=out_specs, check_vma=False)
```

```python
import jax
import jax.numpy as jnp
from jax import lax
from jax.experimental import pallas as pl
from jax.experimental.pallas import tpu as pltpu
from jax.sharding import Mesh
from jax.sharding import PartitionSpec as P


D = 3072
SEQ = 128
EPSILON = 1e-06
F32 = jnp.float32
BF16 = jnp.bfloat16
FS = ("z", "y")
TP = ("x", "c")
ROWS = 192
HALF = ROWS // 2
UNITS = 704
WIDE = 768
TOKS = 512
COLS = 384


VMEM = pl.BlockSpec(memory_space=pltpu.VMEM)
SMEM = pl.BlockSpec(memory_space=pltpu.SMEM)


def moved(value, axis, by):
    return lax.ppermute(value, axis, [(i, (i + by) % 4) for i in range(4)])


def swapped(value):
    return lax.ppermute(value, "c", [(0, 1), (1, 0)])


def gathered(own, axis):
    half = own.shape[0] // 2
    left, right = moved(own, axis, 1), moved(own, axis, -1)
    far_low, far_high = moved(left[:half], axis, 1), moved(right[half:], axis, -1)
    return [own, right, far_low, far_high, left]


def plus(a, b):
    return (a.astype(F32) + b.astype(F32)).astype(BF16)


def reduced(own, after, far_low, far_high, before, axis, out=BF16):
    half = far_low.shape[0]
    from_left, from_right = moved(far_low, axis, 1), moved(far_high, axis, -1)
    to_right = jnp.concatenate([plus(after[:half], from_left), after[half:]], axis=0)
    to_left = jnp.concatenate([before[:half], plus(before[half:], from_right)], axis=0)
    got_left = moved(to_right, axis, 1)
    got_right = moved(to_left, axis, -1)
    return (own.astype(F32) + got_left.astype(F32) + got_right.astype(F32)).astype(out)


def in_five(value):
    n = value.shape[0] // 8
    return (value[: 2 * n], value[2 * n : 4 * n], value[4 * n : 5 * n], value[5 * n : 6 * n], value[6 * n :])


def device_at(where, dz, dy):
    return (where[0] + dz) % 4, (where[1] + dy) % 4


def mix(gate, taps):
    lane = lax.broadcasted_iota(jnp.int32, gate.shape, 1)
    before = jnp.where(lane == 0, 0.0, pltpu.roll(gate, 1, 1))
    after = jnp.where(lane == SEQ - 1, 0.0, pltpu.roll(gate, SEQ - 1, 1))
    mixed = taps[:, 0:1] * before + taps[:, 1:2] * gate + taps[:, 2:3] * after
    return before, after, mixed, jax.nn.sigmoid(mixed)


STEP = 88


def hidden_body(gate_ref, value_ref, taps_ref, hidden_ref):
    for u in range(0, UNITS, STEP):
        rows = slice(u, u + STEP)
        taps = taps_ref[rows, :]
        for t in range(0, TOKS, SEQ):
            cols = slice(t, t + SEQ)
            _, _, mixed, sig = mix(gate_ref[rows, cols].astype(F32), taps)
            hidden_ref[rows, cols] = (mixed * sig * value_ref[rows, cols].astype(F32)).astype(BF16)


def arrange_body(where_ref, *rest):
    refs, (grad_ref, inputs_ref) = rest[:10], rest[10:]
    for c_off in range(2):
        at = 0
        for ref in refs[c_off * 5 : c_off * 5 + 5]:
            rows = ref.shape[0]
            block = (where_ref[2] + at // COLS) % 4 * 2 + (where_ref[3] + c_off) % 2
            to = pl.multiple_of(block * COLS + at % COLS, ROWS)
            grad_ref[pl.ds(to, rows), :] = ref[:, :TOKS]
            inputs_ref[pl.ds(to, rows), :] = ref[:, TOKS:]
            at += rows


def join_body(*refs):
    for k in range(2):
        at = 0
        for ref in refs[k * 5 : k * 5 + 5]:
            rows = ref.shape[0]
            refs[10 + k][at : at + rows, :] = ref[...]
            at += rows


def back_body(down_ref, grad_ref, gate_ref, value_ref, taps_ref, out_ref, sums_ref, act_ref):
    act_ref[...] = lax.dot_general(
        down_ref[:, :UNITS],
        grad_ref[...],
        (((0,), (0,)), ((), ())),
        preferred_element_type=F32,
    )
    for u in range(0, UNITS, STEP):
        rows = slice(u, u + STEP)
        taps = taps_ref[rows, :]
        sums = [jnp.zeros((STEP, SEQ), F32)] * 3
        for t in range(0, TOKS, SEQ):
            cols = slice(t, t + SEQ)
            gate = gate_ref[rows, cols].astype(F32)
            before, after, mixed, sig = mix(gate, taps)
            grad_act = act_ref[rows, cols]
            out_ref[UNITS + u : UNITS + u + STEP, cols] = (grad_act * (mixed * sig)).astype(BF16)
            inner = (
                grad_act * value_ref[rows, cols].astype(F32) * sig * (1.0 + mixed * (1.0 - sig))
            )
            sums = [s + inner * g for s, g in zip(sums, (before, gate, after))]
            lane = lax.broadcasted_iota(jnp.int32, inner.shape, 1)
            following = jnp.where(lane == SEQ - 1, 0.0, pltpu.roll(inner, SEQ - 1, 1))
            previous = jnp.where(lane == 0, 0.0, pltpu.roll(inner, 1, 1))
            out_ref[rows, cols] = (
                taps[:, 1:2] * inner + taps[:, 0:1] * following + taps[:, 2:3] * previous
            ).astype(BF16)
        for k in range(3):
            sums_ref[rows, k : k + 1] = jnp.sum(sums[k], axis=1, keepdims=True)


def product(left, right):
    return lax.dot_general(
        left, right, (((1,), (1,)), ((), ())), preferred_element_type=F32
    ).astype(BF16)


def outer_body(inputs_ref, grad_ref, both_ref, hidden_ref, out_ref):
    out_ref[:, : 2 * UNITS] = product(inputs_ref[...], both_ref[...])
    out_ref[:, 2 * UNITS :] = product(grad_ref[...], hidden_ref[...])


def block_of(refs, dz, dy):
    def part(five, major, minor):
        ref = five[(0, 1, 2 + minor // 2, 4)[major]]
        at = (minor % 2 if major == 2 else minor) * HALF
        return ref[at : at + HALF, :]

    return jnp.concatenate([part(refs[:5], dz, dy), part(refs[5:], dy, dz)], axis=0)


def input_body(where_ref, right_ref, *rest):
    refs, (kept_ref, sent_ref) = rest[:10], rest[10:]
    where = [where_ref[k] for k in range(4)]
    for dz in range(4):
        for dy in range(4):
            zt, yt = device_at(where, dz, dy)
            at = pl.multiple_of((((zt - where[2] + 4) % 4) * 2 + yt % 2) * ROWS, ROWS)
            near = yt // 2 == where[3]
            block = jnp.dot(
                block_of(refs, dz, dy), right_ref[...], preferred_element_type=F32
            ).astype(BF16)

            @pl.when(near)
            def _():
                kept_ref[pl.ds(at, ROWS), :] = block

            @pl.when(jnp.logical_not(near))
            def _():
                sent_ref[pl.ds(at, ROWS), :] = block


PARAMS = pltpu.CompilerParams(vmem_limit_bytes=50 * 1024 * 1024)


def hidden_of(gate, value, taps):
    return pl.pallas_call(
        hidden_body,
        out_shape=jax.ShapeDtypeStruct((UNITS, TOKS), BF16),
        in_specs=[VMEM] * 3,
        out_specs=VMEM,
        compiler_params=PARAMS,
        name="hidden",
    )(gate, value, taps)


def arranged(where, *pieces):
    shape = jax.ShapeDtypeStruct((D, TOKS), BF16)
    return pl.pallas_call(
        arrange_body,
        out_shape=(shape, shape),
        in_specs=[SMEM] + [VMEM] * 10,
        out_specs=(VMEM, VMEM),
        compiler_params=PARAMS,
        name="arrange",
    )(where, *pieces)


def joined(*pieces):
    shape = jax.ShapeDtypeStruct((4 * HALF, 2 * UNITS), BF16)
    return pl.pallas_call(
        join_body,
        out_shape=(shape, shape),
        in_specs=[VMEM] * 10,
        out_specs=(VMEM, VMEM),
        compiler_params=PARAMS,
        name="join",
    )(*pieces)


def back_of(down, grad, gate, value, taps):
    return pl.pallas_call(
        back_body,
        out_shape=(
            jax.ShapeDtypeStruct((2 * UNITS, TOKS), BF16),
            jax.ShapeDtypeStruct((UNITS, 3), F32),
        ),
        in_specs=[VMEM] * 5,
        out_specs=(VMEM, VMEM),
        scratch_shapes=[pltpu.VMEM((UNITS, TOKS), F32)],
        compiler_params=PARAMS,
        cost_estimate=pl.CostEstimate(
            flops=2 * D * UNITS * TOKS, bytes_accessed=12_000_000, transcendentals=UNITS * TOKS
        ),
        name="back",
    )(down, grad, gate, value, taps)


def outer_of(inputs, grad, both, hidden):
    return pl.pallas_call(
        outer_body,
        out_shape=jax.ShapeDtypeStruct((D, 3 * UNITS), BF16),
        grid=(8,),
        in_specs=[
            pl.BlockSpec((COLS, TOKS), lambda i: (i, 0)),
            pl.BlockSpec((COLS, TOKS), lambda i: (i, 0)),
            VMEM,
            VMEM,
        ],
        out_specs=pl.BlockSpec((COLS, 3 * UNITS), lambda i: (i, 0)),
        compiler_params=PARAMS,
        cost_estimate=pl.CostEstimate(
            flops=6 * D * UNITS * TOKS, bytes_accessed=20_000_000, transcendentals=0
        ),
        name="outer",
    )(inputs, grad, both, hidden)


def input_of(where, right, pieces):
    shape = jax.ShapeDtypeStruct((4 * COLS, TOKS), BF16)
    return pl.pallas_call(
        input_body,
        out_shape=(shape, shape),
        in_specs=[SMEM] + [VMEM] * 11,
        out_specs=(VMEM, VMEM),
        compiler_params=PARAMS,
        cost_estimate=pl.CostEstimate(
            flops=4 * D * UNITS * TOKS, bytes_accessed=15_000_000, transcendentals=0
        ),
        name="grad_input",
    )(where, right, *pieces)


def copy_for_each(value, axis):
    copies = jnp.broadcast_to(value, (lax.axis_size(axis), *value.shape))
    return lax.all_to_all(copies, axis, split_axis=0, concat_axis=0, tiled=True)


def over_features(where, own):
    mine = gathered(own, "x")
    other = [None] * 5
    for picks in ((0,), (1, 4), (2, 3)):
        for k in picks:
            other[k] = swapped(mine[k])
    return arranged(where, *mine, *other)


def layer(
    inputs,
    cotangent,
    pre_norm,
    gate_pre,
    value_pre,
    gate_weight,
    value_weight,
    down_weight,
    conv_taps,
    norm_gain,
):
    where = jnp.stack([lax.axis_index(a) for a in ("z", "y", "x", "c")]).astype(jnp.int32)
    down = jnp.pad(down_weight.T, ((0, 0), (0, WIDE - UNITS)))
    down_full = lax.all_gather(down, FS, axis=0, tiled=True)
    weights = jnp.concatenate([gate_weight, value_weight], axis=1)
    top, low = joined(*gathered(weights[:HALF], "y"), *gathered(weights[HALF:], "z"))

    normed = pre_norm.astype(F32)
    cot_float = cotangent.astype(F32)
    scaled = norm_gain[None, :] * cot_float
    sums = jnp.concatenate([jnp.sum(normed * normed, axis=1), jnp.sum(normed * scaled, axis=1)])
    sums = copy_for_each(sums, TP)
    sums = jnp.sum(sums, axis=0)
    inverse = lax.rsqrt(sums[:TOKS] / D + EPSILON)
    cross = sums[TOKS:] / D
    grad_pre = (inverse[:, None] * (scaled - normed * (inverse * inverse * cross)[:, None])).astype(
        BF16
    )
    gain_local = jnp.sum(cot_float * normed * inverse[:, None], axis=0)

    both = jnp.concatenate([grad_pre.T, inputs.T], axis=1)
    grad_full, inputs_full = over_features(where, both)

    gate, value, taps = gate_pre.T, value_pre.T, conv_taps.T
    pieces = (*gathered(top, "z"), *gathered(low, "y"))
    hidden = hidden_of(gate, value, taps)
    grads, taps_local = back_of(down_full, grad_full, gate, value, taps)
    terms = outer_of(inputs_full, grad_full, grads, hidden)
    summed = lax.psum_scatter(terms, FS, scatter_dimension=0, tiled=True).astype(F32)

    kept, sent = input_of(where, grads, pieces)
    paired = plus(kept, swapped(sent))
    grad_input = reduced(*in_five(paired), "x", F32).T.astype(BF16)

    small = jnp.concatenate([taps_local.T.ravel(), gain_local])
    small = jnp.sum(copy_for_each(small, FS), axis=0)
    grad_taps = small[: 3 * UNITS].reshape(3, UNITS)
    grad_gain = small[3 * UNITS :]
    return (
        grad_input,
        summed[:, :UNITS],
        summed[:, UNITS : 2 * UNITS],
        summed[:, 2 * UNITS :].T,
        grad_taps,
        grad_gain,
    )


def solution(mesh):
    split = Mesh(mesh.devices.reshape(4, 4, 4, 2), ("z", "y", "x", "c"))
    in_specs = (
        P(FS, TP),
        P(FS, TP),
        P(FS, TP),
        P(FS, TP),
        P(FS, TP),
        P(FS, TP),
        P(FS, TP),
        P(TP, FS),
        P(None, TP),
        P(TP),
    )
    out_specs = (P(FS, TP), P(FS, TP), P(FS, TP), P(TP, FS), P(None, TP), P(TP))
    return jax.shard_map(layer, mesh=split, in_specs=in_specs, out_specs=out_specs, check_vma=False)
```

```python
import jax
import jax.numpy as jnp
from jax import lax
from jax.experimental import pallas as pl
from jax.experimental.pallas import tpu as pltpu
from jax.sharding import Mesh
from jax.sharding import PartitionSpec as P


D = 3072
SEQ = 128
EPSILON = 1e-06
F32 = jnp.float32
BF16 = jnp.bfloat16
FS = ("z", "y")
TP = ("x", "c")
ROWS = 192
HALF = ROWS // 2
UNITS = 704
WIDE = 768
TOKS = 512
COLS = 384


VMEM = pl.BlockSpec(memory_space=pltpu.VMEM)
SMEM = pl.BlockSpec(memory_space=pltpu.SMEM)


def moved(value, axis, by):
    return lax.ppermute(value, axis, [(i, (i + by) % 4) for i in range(4)])


def swapped(value):
    return lax.ppermute(value, "c", [(0, 1), (1, 0)])


def gathered(own, axis):
    half = own.shape[0] // 2
    left, right = moved(own, axis, 1), moved(own, axis, -1)
    far_low, far_high = moved(left[:half], axis, 1), moved(right[half:], axis, -1)
    return [own, right, far_low, far_high, left]


def plus(a, b):
    return (a.astype(F32) + b.astype(F32)).astype(BF16)


def reduced(own, after, far_low, far_high, before, axis, out=BF16):
    half = far_low.shape[0]
    from_left, from_right = moved(far_low, axis, 1), moved(far_high, axis, -1)
    to_right = jnp.concatenate([plus(after[:half], from_left), after[half:]], axis=0)
    to_left = jnp.concatenate([before[:half], plus(before[half:], from_right)], axis=0)
    got_left = moved(to_right, axis, 1)
    got_right = moved(to_left, axis, -1)
    return (own.astype(F32) + got_left.astype(F32) + got_right.astype(F32)).astype(out)


def in_five(value):
    n = value.shape[0] // 8
    return (value[: 2 * n], value[2 * n : 4 * n], value[4 * n : 5 * n], value[5 * n : 6 * n], value[6 * n :])


def device_at(where, dz, dy):
    return (where[0] + dz) % 4, (where[1] + dy) % 4


def mix(gate, taps):
    lane = lax.broadcasted_iota(jnp.int32, gate.shape, 1)
    before = jnp.where(lane == 0, 0.0, pltpu.roll(gate, 1, 1))
    after = jnp.where(lane == SEQ - 1, 0.0, pltpu.roll(gate, SEQ - 1, 1))
    mixed = taps[:, 0:1] * before + taps[:, 1:2] * gate + taps[:, 2:3] * after
    return before, after, mixed, jax.nn.sigmoid(mixed)


STEP = 88
BACK_STEPS = 4


def hidden_body(gate_ref, value_ref, taps_ref, hidden_ref):
    for u in range(0, UNITS, STEP):
        rows = slice(u, u + STEP)
        taps = taps_ref[rows, :]
        for t in range(0, TOKS, SEQ):
            cols = slice(t, t + SEQ)
            _, _, mixed, sig = mix(gate_ref[rows, cols].astype(F32), taps)
            hidden_ref[rows, cols] = (mixed * sig * value_ref[rows, cols].astype(F32)).astype(BF16)


def arrange_body(where_ref, *rest):
    refs, (grad_ref, inputs_ref) = rest[:10], rest[10:]
    for c_off in range(2):
        at = 0
        for ref in refs[c_off * 5 : c_off * 5 + 5]:
            rows = ref.shape[0]
            block = (where_ref[2] + at // COLS) % 4 * 2 + (where_ref[3] + c_off) % 2
            to = pl.multiple_of(block * COLS + at % COLS, ROWS)
            grad_ref[pl.ds(to, rows), :] = ref[:, :TOKS]
            inputs_ref[pl.ds(to, rows), :] = ref[:, TOKS:]
            at += rows


def join_body(*refs):
    for k in range(2):
        at = 0
        for ref in refs[k * 5 : k * 5 + 5]:
            rows = ref.shape[0]
            refs[10 + k][at : at + rows, :] = ref[...]
            at += rows


def back_body(down_ref, grad_ref, gate_ref, value_ref, taps_ref, out_ref, sums_ref, act_ref):
    step = pl.program_id(0)
    part = lax.dot_general(
        down_ref[:, :UNITS],
        grad_ref[...],
        (((0,), (0,)), ((), ())),
        preferred_element_type=F32,
    )

    @pl.when(step == 0)
    def _():
        act_ref[...] = part

    @pl.when(step > 0)
    def _():
        act_ref[...] += part

    @pl.when(step == BACK_STEPS - 1)
    def _():
        finish_back(gate_ref, value_ref, taps_ref, out_ref, sums_ref, act_ref)


def finish_back(gate_ref, value_ref, taps_ref, out_ref, sums_ref, act_ref):
    for u in range(0, UNITS, STEP):
        rows = slice(u, u + STEP)
        taps = taps_ref[rows, :]
        sums = [jnp.zeros((STEP, SEQ), F32)] * 3
        for t in range(0, TOKS, SEQ):
            cols = slice(t, t + SEQ)
            gate = gate_ref[rows, cols].astype(F32)
            before, after, mixed, sig = mix(gate, taps)
            grad_act = act_ref[rows, cols]
            out_ref[UNITS + u : UNITS + u + STEP, cols] = (grad_act * (mixed * sig)).astype(BF16)
            inner = (
                grad_act * value_ref[rows, cols].astype(F32) * sig * (1.0 + mixed * (1.0 - sig))
            )
            sums = [s + inner * g for s, g in zip(sums, (before, gate, after))]
            lane = lax.broadcasted_iota(jnp.int32, inner.shape, 1)
            following = jnp.where(lane == SEQ - 1, 0.0, pltpu.roll(inner, SEQ - 1, 1))
            previous = jnp.where(lane == 0, 0.0, pltpu.roll(inner, 1, 1))
            out_ref[rows, cols] = (
                taps[:, 1:2] * inner + taps[:, 0:1] * following + taps[:, 2:3] * previous
            ).astype(BF16)
        for k in range(3):
            sums_ref[rows, k : k + 1] = jnp.sum(sums[k], axis=1, keepdims=True)


def product(left, right):
    return lax.dot_general(
        left, right, (((1,), (1,)), ((), ())), preferred_element_type=F32
    ).astype(BF16)


def outer_body(inputs_ref, grad_ref, both_ref, hidden_ref, out_ref):
    out_ref[:, : 2 * UNITS] = product(inputs_ref[...], both_ref[...])
    out_ref[:, 2 * UNITS :] = product(grad_ref[...], hidden_ref[...])


def block_of(refs, dz, dy):
    def part(five, major, minor):
        ref = five[(0, 1, 2 + minor // 2, 4)[major]]
        at = (minor % 2 if major == 2 else minor) * HALF
        return ref[at : at + HALF, :]

    return jnp.concatenate([part(refs[:5], dz, dy), part(refs[5:], dy, dz)], axis=0)


def input_body(where_ref, right_ref, *rest):
    refs, (kept_ref, sent_ref) = rest[:10], rest[10:]
    where = [where_ref[k] for k in range(4)]
    for dz in range(4):
        for dy in range(4):
            zt, yt = device_at(where, dz, dy)
            at = pl.multiple_of((((zt - where[2] + 4) % 4) * 2 + yt % 2) * ROWS, ROWS)
            near = yt // 2 == where[3]
            block = jnp.dot(
                block_of(refs, dz, dy), right_ref[...], preferred_element_type=F32
            ).astype(BF16)

            @pl.when(near)
            def _():
                kept_ref[pl.ds(at, ROWS), :] = block

            @pl.when(jnp.logical_not(near))
            def _():
                sent_ref[pl.ds(at, ROWS), :] = block


PARAMS = pltpu.CompilerParams(vmem_limit_bytes=50 * 1024 * 1024)


def hidden_of(gate, value, taps):
    return pl.pallas_call(
        hidden_body,
        out_shape=jax.ShapeDtypeStruct((UNITS, TOKS), BF16),
        in_specs=[VMEM] * 3,
        out_specs=VMEM,
        compiler_params=PARAMS,
        name="hidden",
    )(gate, value, taps)


def arranged(where, *pieces):
    shape = jax.ShapeDtypeStruct((D, TOKS), BF16)
    return pl.pallas_call(
        arrange_body,
        out_shape=(shape, shape),
        in_specs=[SMEM] + [VMEM] * 10,
        out_specs=(VMEM, VMEM),
        compiler_params=PARAMS,
        name="arrange",
    )(where, *pieces)


def joined(*pieces):
    shape = jax.ShapeDtypeStruct((4 * HALF, 2 * UNITS), BF16)
    return pl.pallas_call(
        join_body,
        out_shape=(shape, shape),
        in_specs=[VMEM] * 10,
        out_specs=(VMEM, VMEM),
        compiler_params=PARAMS,
        name="join",
    )(*pieces)


def back_of(down, grad, gate, value, taps):
    rows = D // BACK_STEPS
    return pl.pallas_call(
        back_body,
        out_shape=(
            jax.ShapeDtypeStruct((2 * UNITS, TOKS), BF16),
            jax.ShapeDtypeStruct((UNITS, 3), F32),
        ),
        grid=(BACK_STEPS,),
        in_specs=[
            pl.BlockSpec((rows, WIDE), lambda i: (i, 0)),
            pl.BlockSpec((rows, TOKS), lambda i: (i, 0)),
            VMEM,
            VMEM,
            VMEM,
        ],
        out_specs=(VMEM, VMEM),
        scratch_shapes=[pltpu.VMEM((UNITS, TOKS), F32)],
        compiler_params=PARAMS,
        cost_estimate=pl.CostEstimate(
            flops=2 * D * UNITS * TOKS, bytes_accessed=12_000_000, transcendentals=UNITS * TOKS
        ),
        name="back",
    )(down, grad, gate, value, taps)


def outer_of(inputs, grad, both, hidden):
    return pl.pallas_call(
        outer_body,
        out_shape=jax.ShapeDtypeStruct((D, 3 * UNITS), BF16),
        grid=(8,),
        in_specs=[
            pl.BlockSpec((COLS, TOKS), lambda i: (i, 0)),
            pl.BlockSpec((COLS, TOKS), lambda i: (i, 0)),
            VMEM,
            VMEM,
        ],
        out_specs=pl.BlockSpec((COLS, 3 * UNITS), lambda i: (i, 0)),
        compiler_params=PARAMS,
        cost_estimate=pl.CostEstimate(
            flops=6 * D * UNITS * TOKS, bytes_accessed=20_000_000, transcendentals=0
        ),
        name="outer",
    )(inputs, grad, both, hidden)


def input_of(where, right, pieces):
    shape = jax.ShapeDtypeStruct((4 * COLS, TOKS), BF16)
    return pl.pallas_call(
        input_body,
        out_shape=(shape, shape),
        in_specs=[SMEM] + [VMEM] * 11,
        out_specs=(VMEM, VMEM),
        compiler_params=PARAMS,
        cost_estimate=pl.CostEstimate(
            flops=4 * D * UNITS * TOKS, bytes_accessed=15_000_000, transcendentals=0
        ),
        name="grad_input",
    )(where, right, *pieces)


def copy_for_each(value, axis):
    copies = jnp.broadcast_to(value, (lax.axis_size(axis), *value.shape))
    return lax.all_to_all(copies, axis, split_axis=0, concat_axis=0, tiled=True)


def over_features(where, own):
    mine = gathered(own, "x")
    other = [None] * 5
    for picks in ((0,), (1, 4), (2, 3)):
        for k in picks:
            other[k] = swapped(mine[k])
    return arranged(where, *mine, *other)


def layer(
    inputs,
    cotangent,
    pre_norm,
    gate_pre,
    value_pre,
    gate_weight,
    value_weight,
    down_weight,
    conv_taps,
    norm_gain,
):
    where = jnp.stack([lax.axis_index(a) for a in ("z", "y", "x", "c")]).astype(jnp.int32)
    down = jnp.pad(down_weight.T, ((0, 0), (0, WIDE - UNITS)))
    down_full = lax.all_gather(down, FS, axis=0, tiled=True)
    weights = jnp.concatenate([gate_weight, value_weight], axis=1)
    top, low = joined(*gathered(weights[:HALF], "y"), *gathered(weights[HALF:], "z"))

    normed = pre_norm.astype(F32)
    cot_float = cotangent.astype(F32)
    scaled = norm_gain[None, :] * cot_float
    sums = jnp.concatenate([jnp.sum(normed * normed, axis=1), jnp.sum(normed * scaled, axis=1)])
    sums = copy_for_each(sums, TP)
    sums = jnp.sum(sums, axis=0)
    inverse = lax.rsqrt(sums[:TOKS] / D + EPSILON)
    cross = sums[TOKS:] / D
    grad_pre = (inverse[:, None] * (scaled - normed * (inverse * inverse * cross)[:, None])).astype(
        BF16
    )
    gain_local = jnp.sum(cot_float * normed * inverse[:, None], axis=0)

    both = jnp.concatenate([grad_pre.T, inputs.T], axis=1)
    grad_full, inputs_full = over_features(where, both)

    gate, value, taps = gate_pre.T, value_pre.T, conv_taps.T
    pieces = (*gathered(top, "z"), *gathered(low, "y"))
    hidden = hidden_of(gate, value, taps)
    grads, taps_local = back_of(down_full, grad_full, gate, value, taps)
    terms = outer_of(inputs_full, grad_full, grads, hidden)
    summed = lax.psum_scatter(terms, FS, scatter_dimension=0, tiled=True).astype(F32)

    kept, sent = input_of(where, grads, pieces)
    paired = plus(kept, swapped(sent))
    grad_input = reduced(*in_five(paired), "x", F32).T.astype(BF16)

    small = jnp.concatenate([taps_local.T.ravel(), gain_local])
    small = jnp.sum(copy_for_each(small, FS), axis=0)
    grad_taps = small[: 3 * UNITS].reshape(3, UNITS)
    grad_gain = small[3 * UNITS :]
    return (
        grad_input,
        summed[:, :UNITS],
        summed[:, UNITS : 2 * UNITS],
        summed[:, 2 * UNITS :].T,
        grad_taps,
        grad_gain,
    )


def solution(mesh):
    split = Mesh(mesh.devices.reshape(4, 4, 4, 2), ("z", "y", "x", "c"))
    in_specs = (
        P(FS, TP),
        P(FS, TP),
        P(FS, TP),
        P(FS, TP),
        P(FS, TP),
        P(FS, TP),
        P(FS, TP),
        P(TP, FS),
        P(None, TP),
        P(TP),
    )
    out_specs = (P(FS, TP), P(FS, TP), P(FS, TP), P(TP, FS), P(None, TP), P(TP))
    return jax.shard_map(layer, mesh=split, in_specs=in_specs, out_specs=out_specs, check_vma=False)
```

```python
import jax
import jax.numpy as jnp
from jax import lax
from jax.experimental import pallas as pl
from jax.experimental.pallas import tpu as pltpu
from jax.sharding import Mesh
from jax.sharding import PartitionSpec as P


D = 3072
SEQ = 128
EPSILON = 1e-06
F32 = jnp.float32
BF16 = jnp.bfloat16
FS = ("z", "y")
TP = ("x", "c")
ROWS = 192
HALF = ROWS // 2
UNITS = 704
WIDE = 768
TOKS = 512
COLS = 384


VMEM = pl.BlockSpec(memory_space=pltpu.VMEM)
SMEM = pl.BlockSpec(memory_space=pltpu.SMEM)


def moved(value, axis, by):
    return lax.ppermute(value, axis, [(i, (i + by) % 4) for i in range(4)])


def swapped(value):
    return lax.ppermute(value, "c", [(0, 1), (1, 0)])


def gathered(own, axis):
    half = own.shape[0] // 2
    left, right = moved(own, axis, 1), moved(own, axis, -1)
    far_low, far_high = moved(left[:half], axis, 1), moved(right[half:], axis, -1)
    return [own, right, far_low, far_high, left]


def plus(a, b):
    return (a.astype(F32) + b.astype(F32)).astype(BF16)


def reduced(own, after, far_low, far_high, before, axis, out=BF16):
    half = far_low.shape[0]
    from_left, from_right = moved(far_low, axis, 1), moved(far_high, axis, -1)
    to_right = jnp.concatenate([plus(after[:half], from_left), after[half:]], axis=0)
    to_left = jnp.concatenate([before[:half], plus(before[half:], from_right)], axis=0)
    got_left = moved(to_right, axis, 1)
    got_right = moved(to_left, axis, -1)
    return (own.astype(F32) + got_left.astype(F32) + got_right.astype(F32)).astype(out)


def in_five(value):
    n = value.shape[0] // 8
    return (value[: 2 * n], value[2 * n : 4 * n], value[4 * n : 5 * n], value[5 * n : 6 * n], value[6 * n :])


def device_at(where, dz, dy):
    return (where[0] + dz) % 4, (where[1] + dy) % 4


def mix(gate, taps):
    lane = lax.broadcasted_iota(jnp.int32, gate.shape, 1)
    before = jnp.where(lane == 0, 0.0, pltpu.roll(gate, 1, 1))
    after = jnp.where(lane == SEQ - 1, 0.0, pltpu.roll(gate, SEQ - 1, 1))
    mixed = taps[:, 0:1] * before + taps[:, 1:2] * gate + taps[:, 2:3] * after
    return before, after, mixed, jax.nn.sigmoid(mixed)


STEP = 88
BACK_STEPS = 2
OUTER_STEPS = 4


def hidden_body(gate_ref, value_ref, taps_ref, hidden_ref):
    for u in range(0, UNITS, STEP):
        rows = slice(u, u + STEP)
        taps = taps_ref[rows, :]
        for t in range(0, TOKS, SEQ):
            cols = slice(t, t + SEQ)
            _, _, mixed, sig = mix(gate_ref[rows, cols].astype(F32), taps)
            hidden_ref[rows, cols] = (mixed * sig * value_ref[rows, cols].astype(F32)).astype(BF16)


def arrange_body(where_ref, *rest):
    refs, (grad_ref, inputs_ref) = rest[:10], rest[10:]
    for c_off in range(2):
        at = 0
        for ref in refs[c_off * 5 : c_off * 5 + 5]:
            rows = ref.shape[0]
            block = (where_ref[2] + at // COLS) % 4 * 2 + (where_ref[3] + c_off) % 2
            to = pl.multiple_of(block * COLS + at % COLS, ROWS)
            grad_ref[pl.ds(to, rows), :] = ref[:, :TOKS]
            inputs_ref[pl.ds(to, rows), :] = ref[:, TOKS:]
            at += rows


def join_body(*refs):
    for k in range(2):
        at = 0
        for ref in refs[k * 5 : k * 5 + 5]:
            rows = ref.shape[0]
            refs[10 + k][at : at + rows, :] = ref[...]
            at += rows


def back_body(down_ref, grad_ref, gate_ref, value_ref, taps_ref, out_ref, sums_ref, act_ref):
    step = pl.program_id(0)
    part = lax.dot_general(
        down_ref[:, :UNITS],
        grad_ref[...],
        (((0,), (0,)), ((), ())),
        preferred_element_type=F32,
    )

    @pl.when(step == 0)
    def _():
        act_ref[...] = part

    @pl.when(step > 0)
    def _():
        act_ref[...] += part

    @pl.when(step == BACK_STEPS - 1)
    def _():
        finish_back(gate_ref, value_ref, taps_ref, out_ref, sums_ref, act_ref)


def finish_back(gate_ref, value_ref, taps_ref, out_ref, sums_ref, act_ref):
    for u in range(0, UNITS, STEP):
        rows = slice(u, u + STEP)
        taps = taps_ref[rows, :]
        sums = [jnp.zeros((STEP, SEQ), F32)] * 3
        for t in range(0, TOKS, SEQ):
            cols = slice(t, t + SEQ)
            gate = gate_ref[rows, cols].astype(F32)
            before, after, mixed, sig = mix(gate, taps)
            grad_act = act_ref[rows, cols]
            out_ref[UNITS + u : UNITS + u + STEP, cols] = (grad_act * (mixed * sig)).astype(BF16)
            inner = (
                grad_act * value_ref[rows, cols].astype(F32) * sig * (1.0 + mixed * (1.0 - sig))
            )
            sums = [s + inner * g for s, g in zip(sums, (before, gate, after))]
            lane = lax.broadcasted_iota(jnp.int32, inner.shape, 1)
            following = jnp.where(lane == SEQ - 1, 0.0, pltpu.roll(inner, SEQ - 1, 1))
            previous = jnp.where(lane == 0, 0.0, pltpu.roll(inner, 1, 1))
            out_ref[rows, cols] = (
                taps[:, 1:2] * inner + taps[:, 0:1] * following + taps[:, 2:3] * previous
            ).astype(BF16)
        for k in range(3):
            sums_ref[rows, k : k + 1] = jnp.sum(sums[k], axis=1, keepdims=True)


def product(left, right):
    return lax.dot_general(
        left, right, (((1,), (1,)), ((), ())), preferred_element_type=F32
    ).astype(BF16)


def outer_body(inputs_ref, grad_ref, both_ref, hidden_ref, out_ref):
    out_ref[:, : 2 * UNITS] = product(inputs_ref[...], both_ref[...])
    out_ref[:, 2 * UNITS :] = product(grad_ref[...], hidden_ref[...])


def block_of(refs, dz, dy):
    def part(five, major, minor):
        ref = five[(0, 1, 2 + minor // 2, 4)[major]]
        at = (minor % 2 if major == 2 else minor) * HALF
        return ref[at : at + HALF, :]

    return jnp.concatenate([part(refs[:5], dz, dy), part(refs[5:], dy, dz)], axis=0)


def input_body(where_ref, right_ref, *rest):
    refs, (kept_ref, sent_ref) = rest[:10], rest[10:]
    where = [where_ref[k] for k in range(4)]
    for dz in range(4):
        for dy in range(4):
            zt, yt = device_at(where, dz, dy)
            at = pl.multiple_of((((zt - where[2] + 4) % 4) * 2 + yt % 2) * ROWS, ROWS)
            near = yt // 2 == where[3]
            block = jnp.dot(
                block_of(refs, dz, dy), right_ref[...], preferred_element_type=F32
            ).astype(BF16)

            @pl.when(near)
            def _():
                kept_ref[pl.ds(at, ROWS), :] = block

            @pl.when(jnp.logical_not(near))
            def _():
                sent_ref[pl.ds(at, ROWS), :] = block


PARAMS = pltpu.CompilerParams(vmem_limit_bytes=50 * 1024 * 1024)


def hidden_of(gate, value, taps):
    return pl.pallas_call(
        hidden_body,
        out_shape=jax.ShapeDtypeStruct((UNITS, TOKS), BF16),
        in_specs=[VMEM] * 3,
        out_specs=VMEM,
        compiler_params=PARAMS,
        name="hidden",
    )(gate, value, taps)


def arranged(where, *pieces):
    shape = jax.ShapeDtypeStruct((D, TOKS), BF16)
    return pl.pallas_call(
        arrange_body,
        out_shape=(shape, shape),
        in_specs=[SMEM] + [VMEM] * 10,
        out_specs=(VMEM, VMEM),
        compiler_params=PARAMS,
        name="arrange",
    )(where, *pieces)


def joined(*pieces):
    shape = jax.ShapeDtypeStruct((4 * HALF, 2 * UNITS), BF16)
    return pl.pallas_call(
        join_body,
        out_shape=(shape, shape),
        in_specs=[VMEM] * 10,
        out_specs=(VMEM, VMEM),
        compiler_params=PARAMS,
        name="join",
    )(*pieces)


def back_of(down, grad, gate, value, taps):
    rows = D // BACK_STEPS
    return pl.pallas_call(
        back_body,
        out_shape=(
            jax.ShapeDtypeStruct((2 * UNITS, TOKS), BF16),
            jax.ShapeDtypeStruct((UNITS, 3), F32),
        ),
        grid=(BACK_STEPS,),
        in_specs=[
            pl.BlockSpec((rows, WIDE), lambda i: (i, 0)),
            pl.BlockSpec((rows, TOKS), lambda i: (i, 0)),
            VMEM,
            VMEM,
            VMEM,
        ],
        out_specs=(VMEM, VMEM),
        scratch_shapes=[pltpu.VMEM((UNITS, TOKS), F32)],
        compiler_params=PARAMS,
        cost_estimate=pl.CostEstimate(
            flops=2 * D * UNITS * TOKS, bytes_accessed=12_000_000, transcendentals=UNITS * TOKS
        ),
        name="back",
    )(down, grad, gate, value, taps)


def outer_of(inputs, grad, both, hidden):
    rows = D // OUTER_STEPS
    return pl.pallas_call(
        outer_body,
        out_shape=jax.ShapeDtypeStruct((D, 3 * UNITS), BF16),
        grid=(OUTER_STEPS,),
        in_specs=[
            pl.BlockSpec((rows, TOKS), lambda i: (i, 0)),
            pl.BlockSpec((rows, TOKS), lambda i: (i, 0)),
            VMEM,
            VMEM,
        ],
        out_specs=pl.BlockSpec((rows, 3 * UNITS), lambda i: (i, 0)),
        compiler_params=PARAMS,
        cost_estimate=pl.CostEstimate(
            flops=6 * D * UNITS * TOKS, bytes_accessed=20_000_000, transcendentals=0
        ),
        name="outer",
    )(inputs, grad, both, hidden)


def widen_body(summed_ref, *outs):
    whole = summed_ref[...].astype(F32)
    for k, out_ref in enumerate(outs):
        out_ref[...] = whole[:, k * UNITS : (k + 1) * UNITS]


def widened(summed):
    rows = ROWS // 2
    shape = jax.ShapeDtypeStruct((ROWS, UNITS), F32)
    return pl.pallas_call(
        widen_body,
        out_shape=(shape,) * 3,
        grid=(2,),
        in_specs=[pl.BlockSpec((rows, 3 * UNITS), lambda i: (i, 0))],
        out_specs=(pl.BlockSpec((rows, UNITS), lambda i: (i, 0)),) * 3,
        compiler_params=PARAMS,
        name="widen",
    )(summed)


def input_of(where, right, pieces):
    shape = jax.ShapeDtypeStruct((4 * COLS, TOKS), BF16)
    return pl.pallas_call(
        input_body,
        out_shape=(shape, shape),
        in_specs=[SMEM] + [VMEM] * 11,
        out_specs=(VMEM, VMEM),
        compiler_params=PARAMS,
        cost_estimate=pl.CostEstimate(
            flops=4 * D * UNITS * TOKS, bytes_accessed=15_000_000, transcendentals=0
        ),
        name="grad_input",
    )(where, right, *pieces)


def copy_for_each(value, axis):
    copies = jnp.broadcast_to(value, (lax.axis_size(axis), *value.shape))
    return lax.all_to_all(copies, axis, split_axis=0, concat_axis=0, tiled=True)


def over_features(where, own):
    mine = gathered(own, "x")
    other = [None] * 5
    for picks in ((0,), (1, 4), (2, 3)):
        for k in picks:
            other[k] = swapped(mine[k])
    return arranged(where, *mine, *other)


def layer(
    inputs,
    cotangent,
    pre_norm,
    gate_pre,
    value_pre,
    gate_weight,
    value_weight,
    down_weight,
    conv_taps,
    norm_gain,
):
    where = jnp.stack([lax.axis_index(a) for a in ("z", "y", "x", "c")]).astype(jnp.int32)
    down = jnp.pad(down_weight.T, ((0, 0), (0, WIDE - UNITS)))
    down_full = lax.all_gather(down, FS, axis=0, tiled=True)
    weights = jnp.concatenate([gate_weight, value_weight], axis=1)
    top, low = joined(*gathered(weights[:HALF], "y"), *gathered(weights[HALF:], "z"))

    normed = pre_norm.astype(F32)
    cot_float = cotangent.astype(F32)
    scaled = norm_gain[None, :] * cot_float
    sums = jnp.concatenate([jnp.sum(normed * normed, axis=1), jnp.sum(normed * scaled, axis=1)])
    sums = copy_for_each(sums, TP)
    sums = jnp.sum(sums, axis=0)
    inverse = lax.rsqrt(sums[:TOKS] / D + EPSILON)
    cross = sums[TOKS:] / D
    grad_pre = (inverse[:, None] * (scaled - normed * (inverse * inverse * cross)[:, None])).astype(
        BF16
    )
    gain_local = jnp.sum(cot_float * normed * inverse[:, None], axis=0)

    both = jnp.concatenate([grad_pre.T, inputs.T], axis=1)
    grad_full, inputs_full = over_features(where, both)

    gate, value, taps = gate_pre.T, value_pre.T, conv_taps.T
    pieces = (*gathered(top, "z"), *gathered(low, "y"))
    hidden = hidden_of(gate, value, taps)
    grads, taps_local = back_of(down_full, grad_full, gate, value, taps)
    terms = outer_of(inputs_full, grad_full, grads, hidden)
    summed = lax.psum_scatter(terms, FS, scatter_dimension=0, tiled=True)
    grad_gate, grad_value, grad_down = widened(summed)

    kept, sent = input_of(where, grads, pieces)
    paired = plus(kept, swapped(sent))
    grad_input = reduced(*in_five(paired), "x", F32).T.astype(BF16)

    small = jnp.concatenate([taps_local.T.ravel(), gain_local])
    small = jnp.sum(copy_for_each(small, FS), axis=0)
    grad_taps = small[: 3 * UNITS].reshape(3, UNITS)
    grad_gain = small[3 * UNITS :]
    return (
        grad_input,
        grad_gate,
        grad_value,
        grad_down.T,
        grad_taps,
        grad_gain,
    )


def solution(mesh):
    split = Mesh(mesh.devices.reshape(4, 4, 4, 2), ("z", "y", "x", "c"))
    in_specs = (
        P(FS, TP),
        P(FS, TP),
        P(FS, TP),
        P(FS, TP),
        P(FS, TP),
        P(FS, TP),
        P(FS, TP),
        P(TP, FS),
        P(None, TP),
        P(TP),
    )
    out_specs = (P(FS, TP), P(FS, TP), P(FS, TP), P(TP, FS), P(None, TP), P(TP))
    return jax.shard_map(layer, mesh=split, in_specs=in_specs, out_specs=out_specs, check_vma=False)
```
